32 devices in a mesh: sp: 16 (over z, y, x), tp: 2 (over core).
Axes of the slice: x: 2, y: 2, z: 4, core: 2. Of those that a mesh axis runs over, the one named last changes fastest.
Arguments:
- hidden: bfloat16 [4096, 2048], P('sp', 'tp'), may hold values from -16 to 16
- query_weight: bfloat16 [2048, 1024], P(None, 'tp'), may hold values from -0.125 to 0.125
- key_weight: bfloat16 [2048, 512], P(None, 'tp'), may hold values from -0.125 to 0.125
- value_weight: bfloat16 [2048, 512], P(None, 'tp'), may hold values from -0.125 to 0.125
- head_gate_weight: bfloat16 [2048, 1024], P(None, 'tp'), may hold values from -0.125 to 0.125
- state_in_weight: bfloat16 [2048, 1024], P(None, 'tp'), may hold values from -0.125 to 0.125
- state_gate_weight: bfloat16 [2048, 1024], P(None, 'tp'), may hold values from -0.125 to 0.125
- sink_logit: float32 [16], P('tp'), may hold values from 1 to 6
- decay_real: float32 [64, 64], P('tp'), may hold values from -0.7 to -0.0049
- decay_frequency: float32 [64, 64], P('tp'), may hold values from 0 to 192
- log_step: float32 [64], P('tp'), may hold values from -20 to 0
- input_real: float32 [64, 64, 16], P('tp'), may hold values from -1028 to 1028
- input_imaginary: float32 [64, 64, 16], P('tp'), may hold values from -1028 to 1028
- output_real: float32 [64, 16, 64], P('tp'), may hold values from -0.5 to 0.5
- output_imaginary: float32 [64, 16, 64], P('tp'), may hold values from -0.5 to 0.5
- skip_weight: float32 [64, 16], P('tp'), may hold values from -3 to 3
- decay_shift: float32 [64, 4096], P('tp', 'sp'), may hold values from -2 to 0
- head_out_weight: bfloat16 [1024, 2048], P('tp'), may hold values from -0.375 to 0.375
- state_out_weight: bfloat16 [1024, 2048], P('tp'), may hold values from -0.375 to 0.375
Outputs:
- layer_out: bfloat16 [4096, 2048], P('sp', 'tp')
The draws below stay inside these ranges and needn't reach their ends.
All inputs are finite; a program needn't handle non-finite values.
Results may differ from the reference program's by a relative error of at most 0.012.
Values may be sent and summed in bfloat16 or wider, within the bound.
A program may use at most 128 MiB of HBM per device.

```python
import math
import jax
import jax.numpy as jnp
from jax import lax

D = 2048
HEAD_DIM = 64
Q_HEADS = 16
KV_HEADS = 8
SSM_GROUPS = 64
GROUP_CH = 16
SSM_STATE = 64
WINDOW = 128
TOK_DEV = 256
TOKENS = 4096
ATT_WIDTH = 1024
KV_WIDTH = 512
SSM_WIDTH = 1024
N_SP = 16


def group_law(key):
    base_key = jax.random.fold_in(key, 101)
    rank_key, slow_key, fast_key, level_key = jax.random.split(base_key, 4)
    fast_count = SSM_GROUPS // 2
    ranks = jax.random.permutation(rank_key, SSM_GROUPS)
    is_fast = ranks < fast_count
    reach = min(100, TOK_DEV // 2)
    slow_log = jax.random.uniform(slow_key, (SSM_GROUPS,), jnp.float32, math.log(7.0 / TOKENS), math.log(30.0 / TOKENS))
    fast_log = jax.random.uniform(fast_key, (SSM_GROUPS,), jnp.float32, math.log(2.0 / reach), math.log(5.0 / reach))
    log_dt = jnp.where(is_fast, fast_log, slow_log)
    level = jax.random.uniform(level_key, (SSM_GROUPS, SSM_STATE), jnp.float32, 0.3, 0.7)
    slow_real = -level * 0.5 / (jnp.exp(slow_log) * TOKENS)[:, None]
    real_part = jnp.where(is_fast[:, None], -level, slow_real)
    return (log_dt, real_part)


def draw_log_step(key, part):
    return group_law(key)[0]


def draw_decay_real(key, part):
    return group_law(key)[1]


def input_draw(key, salt):
    log_dt, real_part = group_law(key)
    draw_key = jax.random.fold_in(key, salt)
    shape = (SSM_GROUPS, SSM_STATE, GROUP_CH)
    raw = jnp.clip(jax.random.normal(draw_key, shape, jnp.float32), -4.0, 4.0)
    scale = (2.0 * GROUP_CH) ** (-0.5) * jnp.sqrt(2.0 * jnp.abs(real_part) / jnp.exp(log_dt)[:, None])
    return raw * scale[:, :, None]


def draw_input_real(key, part):
    return input_draw(key, 202)


def draw_input_imaginary(key, part):
    return input_draw(key, 203)


def draw_decay_shift(key, part):
    rate_key, jitter_key, where_key, amount_key = jax.random.split(jax.random.fold_in(key, 303), 4)
    block_count = TOKENS // TOK_DEV
    block_rate = jnp.exp(jax.random.uniform(rate_key, (block_count,), jnp.float32, math.log(0.2), math.log(0.8))) / TOKENS
    frequency_ratio = jnp.repeat(block_rate, TOK_DEV)
    random_perturbation = jax.random.uniform(jitter_key, (SSM_GROUPS, TOKENS), jnp.float32, 0.5, 1.5)
    places = jax.random.randint(where_key, (SSM_GROUPS, 2), 0, TOKENS)
    total_quantity = jnp.log(jax.random.uniform(amount_key, (SSM_GROUPS, 2), jnp.float32, 0.5, 0.8))
    positions = jnp.arange(TOKENS, dtype=jnp.int32)
    match_count = (places[:, :, None] == positions[None, None, :]).astype(jnp.float32)
    spike_length = jnp.sum(match_count * total_quantity[:, :, None], axis=1)
    return -frequency_ratio[None, :] * random_perturbation + spike_length


def draw_hidden(key, part):
    noise_key = jax.random.fold_in(jax.random.fold_in(key, 404), 0)
    return jnp.clip(jax.random.normal(noise_key, (TOKENS, D), jnp.float32), -6.0, 6.0).astype(jnp.bfloat16)


def block_scale(rng, dims, shards, least, top_value):
    level, own = 1.0, jax.random.fold_in(rng, 6)
    for position, shards_of in shards:
        draws = jnp.exp(jax.random.uniform(jax.random.fold_in(own, position), (shards_of,), jnp.float32, least / len(shards), top_value / len(shards)))
        level = level * jnp.repeat(draws, dims[position] // shards_of).reshape([-1 if axis == position else 1 for axis in range(len(dims))])
    return level


def gaussian(own_key, shape, width, most, cuts=(), held_as=jnp.bfloat16):
    drawn = jax.random.normal(own_key, shape, jnp.float32) * width
    if len(cuts) > 0:
        drawn = block_scale(own_key, shape, cuts, -0.22, 0.18) * drawn
    return jnp.clip(drawn, min=-most, max=most).astype(held_as)


def setup_inputs(seed: int = 0) -> dict:
    key_of = jax.random.split(jax.random.key(seed), 20)
    return {
        "hidden": draw_hidden(jax.random.fold_in(key_of[19], 71), 0),
        "query_weight": gaussian(key_of[1], (D, ATT_WIDTH), D ** -0.5, 0.125, ((1, 2),)),
        "key_weight": gaussian(key_of[2], (D, KV_WIDTH), D ** -0.5, 0.125, ((1, 2),)),
        "value_weight": gaussian(key_of[3], (D, KV_WIDTH), D ** -0.5, 0.125, ((1, 2),)),
        "head_gate_weight": gaussian(key_of[4], (D, ATT_WIDTH), D ** -0.5, 0.125, ((1, 2),)),
        "state_in_weight": gaussian(key_of[5], (D, SSM_WIDTH), D ** -0.5, 0.125, ((1, 2),)),
        "state_gate_weight": gaussian(key_of[6], (D, SSM_WIDTH), D ** -0.5, 0.125, ((1, 2),)),
        "sink_logit": jnp.clip(1.0 + 5.0 * jax.random.uniform(key_of[7], (Q_HEADS,), jnp.float32) ** block_scale(key_of[7], (Q_HEADS,), ((0, 2),), -0.2, 0.2), 1.0, 6.0),
        "decay_real": draw_decay_real(jax.random.fold_in(key_of[19], 71), 0),
        "decay_frequency": jnp.clip(192.0 * jax.random.uniform(key_of[9], (SSM_GROUPS, SSM_STATE), jnp.float32) ** block_scale(key_of[9], (SSM_GROUPS, SSM_STATE), ((0, 2),), -0.2, 0.2), 0.0, 192.0),
        "log_step": draw_log_step(jax.random.fold_in(key_of[19], 71), 0),
        "input_real": draw_input_real(jax.random.fold_in(key_of[19], 71), 0),
        "input_imaginary": draw_input_imaginary(jax.random.fold_in(key_of[19], 71), 0),
        "output_real": gaussian(key_of[13], (SSM_GROUPS, GROUP_CH, SSM_STATE), (2 * SSM_STATE) ** -0.5, 0.5, ((0, 2),), jnp.float32),
        "output_imaginary": gaussian(key_of[14], (SSM_GROUPS, GROUP_CH, SSM_STATE), (2 * SSM_STATE) ** -0.5, 0.5, ((0, 2),), jnp.float32),
        "skip_weight": gaussian(key_of[15], (SSM_GROUPS, GROUP_CH), 0.5, 3.0, ((0, 2),), jnp.float32),
        "decay_shift": draw_decay_shift(jax.random.fold_in(key_of[19], 71), 0),
        "head_out_weight": gaussian(key_of[17], (ATT_WIDTH, D), (ATT_WIDTH // 4) ** -0.5, 0.375, ((0, 2),)),
        "state_out_weight": gaussian(key_of[18], (SSM_WIDTH, D), (SSM_WIDTH // 4) ** -0.5, 0.375, ((0, 2),)),
    }


NEG_FILL = -1e30


def combine(earlier_pair, later_pair):
    prior_real, prior_imag, prior_sum_real, prior_sum_imag = earlier_pair
    after_real, after_imag, after_sum_real, after_sum_imag = later_pair
    return (prior_real * after_real - prior_imag * after_imag,
            prior_real * after_imag + prior_imag * after_real,
            after_real * prior_sum_real - after_imag * prior_sum_imag + after_sum_real,
            after_real * prior_sum_imag + after_imag * prior_sum_real + after_sum_imag)


def band_rows(rows):
    padded = jnp.concatenate([jnp.zeros_like(rows[:1]), rows], axis=0)
    return jnp.concatenate([padded[:-1], padded[1:]], axis=1)


def attention(query_rows_all, key_rows, value_rows, sink_logit):
    blocks = TOKENS // WINDOW
    group_size = Q_HEADS // KV_HEADS
    query_heads = query_rows_all.reshape(blocks, WINDOW, KV_HEADS, group_size, HEAD_DIM).transpose(2, 0, 1, 3, 4)
    key_heads = band_rows(key_rows.reshape(blocks, WINDOW, KV_HEADS, HEAD_DIM)).transpose(2, 0, 1, 3)
    value_heads = band_rows(value_rows.reshape(blocks, WINDOW, KV_HEADS, HEAD_DIM)).transpose(2, 0, 1, 3)
    sink_table = sink_logit.reshape(KV_HEADS, group_size)
    query_index = jnp.arange(WINDOW, dtype=jnp.int32)[:, None]
    column = jnp.arange(2 * WINDOW, dtype=jnp.int32)[None, :]
    distance = WINDOW + query_index - column
    block_start = (jnp.arange(blocks, dtype=jnp.int32) * WINDOW)[:, None, None]
    allowed = (distance >= 0) & (distance < WINDOW) & (block_start - WINDOW + column >= 0)

    def one_head(operands):
        query_part, key_portion_slice, value_part, sink_part = operands
        scores = jnp.einsum('nqgd,nsd->ngqs', query_part.astype(jnp.float32),
                            key_portion_slice.astype(jnp.float32)) * (HEAD_DIM ** -0.5)
        scores = jnp.where(allowed[:, None], scores, NEG_FILL)
        sink_col = sink_part[None, :, None, None]
        maxima = jnp.maximum(jnp.max(scores, axis=-1, keepdims=True), sink_col)
        exponent = jnp.exp(scores - maxima)
        totals = jnp.sum(exponent, axis=-1, keepdims=True) + jnp.exp(sink_col - maxima)
        weights = (exponent / totals).astype(jnp.bfloat16)
        return jnp.einsum('ngqs,nsd->nqgd', weights.astype(jnp.float32), value_part.astype(jnp.float32))

    outputs = lax.map(one_head, (query_heads, key_heads, value_heads, sink_table))
    return outputs.transpose(1, 2, 0, 3, 4).reshape(TOKENS, ATT_WIDTH)


def state_branch(state_input, decay_real, decay_frequency, log_step, input_real, input_imaginary,
                 output_real, output_imaginary, skip_weight, decay_shift):
    highest = lax.Precision.HIGHEST
    stepsize = jnp.exp(log_step)[:, None]
    magnitude = jnp.exp(decay_real * stepsize)
    base_real = magnitude * jnp.cos(decay_frequency * stepsize)
    base_imag = magnitude * jnp.sin(decay_frequency * stepsize)
    denominator = decay_real * decay_real + decay_frequency * decay_frequency
    less_real = base_real - 1.0
    zoh_real = (less_real * decay_real + base_imag * decay_frequency) / denominator
    zoh_imag = (base_imag * decay_real - less_real * decay_frequency) / denominator
    drive_real = zoh_real[..., None] * input_real - zoh_imag[..., None] * input_imaginary
    drive_imag = zoh_real[..., None] * input_imaginary + zoh_imag[..., None] * input_real
    values = state_input.astype(jnp.float32).reshape(N_SP, TOK_DEV, SSM_GROUPS, GROUP_CH)
    shifts = decay_shift.reshape(SSM_GROUPS, N_SP, TOK_DEV).transpose(1, 0, 2)

    def advance(carried, operands):
        carry_real, carry_imag = carried
        block_rows, shift_rows = operands
        push_real = jnp.einsum('tgp,gnp->gnt', block_rows, drive_real, precision=highest)
        push_imag = jnp.einsum('tgp,gnp->gnt', block_rows, drive_imag, precision=highest)
        factor = jnp.exp(shift_rows)[:, None, :]
        cum_real, cum_imag, local_real, local_imag = lax.associative_scan(
            combine, (factor * base_real[..., None], factor * base_imag[..., None], push_real, push_imag), axis=2)
        state_real = local_real + cum_real * carry_real[..., None] - cum_imag * carry_imag[..., None]
        state_imag = local_imag + cum_real * carry_imag[..., None] + cum_imag * carry_real[..., None]
        recurrent = (jnp.einsum('gpn,gnt->tgp', output_real, state_real, precision=highest)
                     - jnp.einsum('gpn,gnt->tgp', output_imaginary, state_imag, precision=highest)
                     + skip_weight[None] * block_rows)
        return (state_real[..., -1], state_imag[..., -1]), recurrent

    zero_state = jnp.zeros((SSM_GROUPS, SSM_STATE), jnp.float32)
    _, outputs = lax.scan(advance, (zero_state, zero_state), (values, shifts))
    return outputs.reshape(TOKENS, SSM_WIDTH)


def reference(hidden, query_weight, key_weight, value_weight, head_gate_weight, state_in_weight,
              state_gate_weight, sink_logit, decay_real, decay_frequency, log_step, input_real,
              input_imaginary, output_real, output_imaginary, skip_weight, decay_shift,
              head_out_weight, state_out_weight):
    def project(weight):
        return jnp.dot(hidden, weight, preferred_element_type=jnp.float32).astype(jnp.bfloat16)

    query_rows_all = project(query_weight)
    key_rows = project(key_weight)
    value_rows = project(value_weight)
    head_gate = project(head_gate_weight)
    state_input = project(state_in_weight)
    state_gate = project(state_gate_weight)
    attended = attention(query_rows_all, key_rows, value_rows, sink_logit)
    head_mixed = (jax.nn.sigmoid(head_gate.astype(jnp.float32)) * attended).astype(jnp.bfloat16)
    recurrent = state_branch(state_input, decay_real, decay_frequency, log_step, input_real,
                             input_imaginary, output_real, output_imaginary, skip_weight, decay_shift)
    state_mixed = (jax.nn.sigmoid(state_gate.astype(jnp.float32)) * jax.nn.gelu(recurrent)).astype(jnp.bfloat16)
    totals = (jnp.dot(head_mixed, head_out_weight, preferred_element_type=jnp.float32)
              + jnp.dot(state_mixed, state_out_weight, preferred_element_type=jnp.float32))
    return totals.astype(jnp.bfloat16)
```

```python
import functools

import jax
import jax.numpy as jnp
import numpy as np
from jax import lax
from jax.experimental import pallas as pl
from jax.experimental.pallas import tpu as pltpu
from jax.sharding import PartitionSpec as P

HEAD_DIM = 64
Q_HEADS = 16
KV_HEADS = 8
GROUP_CH = 16
WINDOW = 128
CHUNK = 16
LANES = 128

NEG_FILL = -1e30
MESH = pl.DeviceIdType.MESH
VMEM = pl.BlockSpec(memory_space=pltpu.VMEM)
BF16 = jnp.bfloat16
F32 = jnp.float32


def shifted(value, axis, steps):
    count = lax.axis_size(axis)
    first, last = (max(0, -steps), min(count, count - steps))
    return lax.ppermute(value, axis, [(source, source + steps) for source in range(first, last)])


def params(collective_id=None):
    extra = {} if collective_id is None else {"collective_id": collective_id, "has_side_effects": True}
    return pltpu.CompilerParams(vmem_limit_bytes=60 * 1024 * 1024, **extra)


def hidden_kernel(own_ref, full_ref, send_sem, recv_sem):
    me = lax.axis_index("tp")
    other = 1 - me
    width = own_ref.shape[1]
    barrier = pltpu.get_barrier_semaphore()
    pl.semaphore_signal(barrier, inc=1, device_id={"tp": other}, device_id_type=MESH)
    pl.semaphore_wait(barrier, 1)
    mine = pl.ds(pl.multiple_of(me * width, LANES), width)
    copy = pltpu.make_async_remote_copy(
        src_ref=own_ref,
        dst_ref=full_ref.at[:, mine],
        send_sem=send_sem,
        recv_sem=recv_sem,
        device_id={"tp": other},
        device_id_type=MESH,
    )
    copy.start()
    full_ref[:, mine] = own_ref[...]
    copy.wait()


def gather_hidden(hidden):
    rows, width = hidden.shape
    return pl.pallas_call(
        hidden_kernel,
        out_shape=jax.ShapeDtypeStruct((rows, 2 * width), hidden.dtype),
        in_specs=[VMEM],
        out_specs=VMEM,
        scratch_shapes=[pltpu.SemaphoreType.DMA, pltpu.SemaphoreType.DMA],
        compiler_params=params(0),
        name="hidden_exchange",
    )(hidden)


def output_kernel(head_ref, state_ref, how_ref, sow_ref, out_ref, away, landed, send_sem, recv_sem):
    me = lax.axis_index("tp")
    other = 1 - me
    rows, width = out_ref.shape
    pieces = away.shape[0]
    step = width // pieces
    barrier = pltpu.get_barrier_semaphore()
    pl.semaphore_signal(barrier, inc=1, device_id={"tp": other}, device_id_type=MESH)
    pl.semaphore_wait(barrier, 1)

    def product(owner, piece):
        columns = pl.ds(pl.multiple_of(owner * width + piece * step, LANES), step)
        return jnp.dot(head_ref[...], how_ref[:, columns], preferred_element_type=F32) + jnp.dot(
            state_ref[...], sow_ref[:, columns], preferred_element_type=F32
        )

    copies = [
        pltpu.make_async_remote_copy(
            src_ref=away.at[piece],
            dst_ref=landed.at[piece],
            send_sem=send_sem.at[piece],
            recv_sem=recv_sem.at[piece],
            device_id={"tp": other},
            device_id_type=MESH,
        )
        for piece in range(pieces)
    ]
    for piece in range(pieces):
        away[piece] = product(other, piece).astype(away.dtype)
        if piece > 0:
            copies[piece - 1].start()
    own = [product(me, 0)]
    copies[pieces - 1].start()
    for piece in range(pieces):
        total = own[0] if piece == 0 else product(me, piece)
        copies[piece].wait()
        out_ref[:, pl.ds(piece * step, step)] = (total + landed[piece].astype(F32)).astype(out_ref.dtype)


def project_out(head_mixed, state_mixed, head_out_weight, state_out_weight):
    rows = head_mixed.shape[0]
    width = head_out_weight.shape[1] // 2
    pieces = 4
    return pl.pallas_call(
        output_kernel,
        out_shape=jax.ShapeDtypeStruct((rows, width), BF16),
        in_specs=[VMEM] * 4,
        out_specs=VMEM,
        scratch_shapes=[
            pltpu.VMEM((pieces, rows, width // pieces), F32),
            pltpu.VMEM((pieces, rows, width // pieces), F32),
            pltpu.SemaphoreType.DMA((pieces,)),
            pltpu.SemaphoreType.DMA((pieces,)),
        ],
        compiler_params=params(1),
        name="output_projection",
    )(head_mixed, state_mixed, head_out_weight, state_out_weight)


def turn(value, same, swapped):
    return value * same + pltpu.roll(value, value.shape[1] // 2, 1) * swapped


def local_kernel(
    uw_ref, gtab_ref, dtab_ref, e_ref, et_ref, a16_ref, b16_ref, tail_ref, whole_ref, tile_ref,
    intra_ref, g_ref, pushed_ref, msg_ref,
):
    groups = gtab_ref.shape[0]
    chunks = uw_ref.shape[0] // groups
    span = uw_ref.shape[1]
    row = lax.broadcasted_iota(jnp.int32, (span, span), 0) // GROUP_CH
    column = lax.broadcasted_iota(jnp.int32, (span, span), 1) // GROUP_CH
    causal = row <= column
    batch = 4

    def one(step, carry):
        ids = [step * batch + k for k in range(batch)]
        wide = [jnp.dot(gtab_ref[g], e_ref[...], preferred_element_type=F32) for g in ids]
        tall = [jnp.dot(et_ref[...], dtab_ref[g], preferred_element_type=F32) for g in ids]
        out_side = [
            (x[:, :span] * x[:, span : 2 * span] + x[:, 2 * span : 3 * span] * x[:, 3 * span :]).astype(BF16)
            for x in wide
        ]
        in_side = [
            (x[:span] * x[span : 2 * span] + x[2 * span : 3 * span] * x[3 * span :]).astype(BF16)
            for x in tall
        ]
        for g, value in zip(ids, out_side):
            g_ref[g] = value
        table = [
            jnp.where(causal, jnp.dot(a, b, preferred_element_type=F32), 0.0).astype(BF16)
            for a, b in zip(in_side, out_side)
        ]
        for g, t, d in zip(ids, table, in_side):
            rows = pl.ds(pl.multiple_of(g * chunks, chunks), chunks)
            u = uw_ref[rows, :]
            intra_ref[rows, :] = jnp.dot(u, t, preferred_element_type=F32)
            pushed_ref[rows, :] = jnp.dot(u, d, preferred_element_type=F32)
        return carry

    lax.fori_loop(0, groups // batch, one, 0)
    same, swapped = a16_ref[...], b16_ref[...]
    state = jnp.zeros((groups, pushed_ref.shape[1]), F32)
    for c in range(chunks):
        rows = pl.ds(c, groups, stride=chunks)
        local = tail_ref[rows, :] * turn(pushed_ref[rows, :], same, swapped)
        pushed_ref[rows, :] = local
        state = whole_ref[rows, :] * turn(state, same, swapped) + local
    msg_ref[:groups, :] = state
    msg_ref[groups:, :] = tile_ref[...]


def carry_kernel(msg_ref, same_ref, swapped_ref, carry_ref, landed, send_sem, recv_sem):
    me = lax.axis_index("sp")
    count = lax.axis_size("sp")
    groups = carry_ref.shape[0]
    barrier = pltpu.get_barrier_semaphore()

    def greet(hop, x):
        pl.semaphore_signal(
            barrier, inc=1, device_id={"sp": lax.rem(me + hop, count)}, device_id_type=MESH
        )
        return x

    lax.fori_loop(1, count, greet, 0)
    pl.semaphore_wait(barrier, count - 1)

    def outgoing(target):
        return pltpu.make_async_remote_copy(
            src_ref=msg_ref,
            dst_ref=landed.at[me],
            send_sem=send_sem.at[target],
            recv_sem=recv_sem.at[me],
            device_id={"sp": target},
            device_id_type=MESH,
        )

    def incoming(source):
        return pltpu.make_async_remote_copy(
            src_ref=msg_ref,
            dst_ref=landed.at[source],
            send_sem=send_sem.at[source],
            recv_sem=recv_sem.at[source],
            device_id={"sp": source},
            device_id_type=MESH,
        )

    def send(target, x):
        outgoing(target).start()
        return x

    lax.fori_loop(me + 1, count, send, 0)
    same, swapped = same_ref[...], swapped_ref[...]
    pick = lax.broadcasted_iota(jnp.int32, (groups, LANES), 0) == lax.broadcasted_iota(
        jnp.int32, (groups, LANES), 1
    )

    def absorb(source, state):
        incoming(source).wait_recv()
        shift_row = landed[source, pl.ds(groups, 1), :]
        total = jnp.sum(jnp.where(pick, shift_row, 0.0), axis=1, keepdims=True)
        return jnp.exp(total) * turn(state, same, swapped) + landed[source, pl.ds(0, groups), :]

    carry_ref[...] = lax.fori_loop(0, me, absorb, jnp.zeros(carry_ref.shape, F32))

    def drain(target, x):
        outgoing(target).wait_send()
        return x

    lax.fori_loop(me + 1, count, drain, 0)


def finish_kernel(
    carry_ref, pushed_ref, intra_ref, g_ref, wout_ref, a16_ref, b16_ref, head_ref, whole_ref,
    out_ref, entry,
):
    groups = g_ref.shape[0]
    chunks = pushed_ref.shape[0] // groups
    same, swapped = a16_ref[...], b16_ref[...]
    state = carry_ref[...]
    for c in range(chunks):
        rows = pl.ds(c, groups, stride=chunks)
        entry[rows, :] = head_ref[rows, :] * state
        state = whole_ref[rows, :] * turn(state, same, swapped) + pushed_ref[rows, :]
    batch = 8

    def one(step, x):
        for k in range(batch):
            g = step * batch + k
            rows = pl.ds(pl.multiple_of(g * chunks, chunks), chunks)
            far = jnp.dot(entry[rows, :].astype(BF16), g_ref[g], preferred_element_type=F32)
            out_ref[rows, :] = (wout_ref[rows, :] * (intra_ref[rows, :] + far)).astype(out_ref.dtype)
        return x

    lax.fori_loop(0, groups // batch, one, 0)


def spread_matrix():
    span = CHUNK * GROUP_CH
    column = np.arange(span)
    by_step = (np.arange(CHUNK)[:, None] == column[None] // GROUP_CH).astype(np.float32)
    by_channel = (np.arange(GROUP_CH)[:, None] == column[None] % GROUP_CH).astype(np.float32)
    out = np.zeros((8 * CHUNK, 4 * span), np.float32)
    for kind in range(4):
        block = by_channel if kind % 2 else by_step
        for half in range(2):
            first = (2 * kind + half) * CHUNK
            out[first : first + CHUNK, kind * span : (kind + 1) * span] = block
    return out


def shift_matrix(states2):
    span = CHUNK * GROUP_CH
    step = np.arange(CHUNK)
    upto = (step[:, None] <= (np.arange(span) // GROUP_CH)[None]).astype(np.float32)
    ref = (step < CHUNK // 2).astype(np.float32)[:, None]
    relative = upto - ref
    return np.concatenate(
        [relative, np.repeat(ref, states2, 1), np.ones((CHUNK, states2), np.float32)], axis=1
    )


def halves(value):
    high = lax.reduce_precision(value, 8, 7)
    return [high.astype(BF16), (value - high).astype(BF16)]


def tables(decay_real, decay_frequency, log_step, input_real, input_imaginary, output_real, output_imaginary, chunks):
    stepsize = jnp.exp(log_step)[:, None]
    log_magnitude = decay_real * stepsize
    rotation = decay_frequency * stepsize
    magnitude = jnp.exp(log_magnitude)
    base_real = magnitude * jnp.cos(rotation)
    base_imag = magnitude * jnp.sin(rotation)
    denominator = decay_real * decay_real + decay_frequency * decay_frequency
    less_real = base_real - 1.0
    zoh_real = (less_real * decay_real + base_imag * decay_frequency) / denominator
    zoh_imag = (base_imag * decay_real - less_real * decay_frequency) / denominator
    counter = jnp.arange(1, CHUNK + 1, dtype=F32)[:, None, None]
    angle = counter * rotation
    cosine, sine = jnp.cos(angle), jnp.sin(angle)
    grow = jnp.exp(counter * log_magnitude)
    shrink = jnp.exp(-counter * log_magnitude)
    power_real, power_imag = grow * cosine, grow * sine
    inverse_real, inverse_imag = shrink * cosine, -shrink * sine
    real_t = power_real.transpose(1, 2, 0)
    imag_t = power_imag.transpose(1, 2, 0)
    out_real = output_real.transpose(0, 2, 1)
    out_imag = output_imaginary.transpose(0, 2, 1)
    stack = lambda a, b: jnp.concatenate([a, b], axis=1)
    x1 = stack(real_t, -imag_t)
    x2 = stack(out_real, out_real)
    x3 = stack(-imag_t, -real_t)
    x4 = stack(out_imag, out_imag)
    gtab = jnp.concatenate([h for x in (x1, x2, x3, x4) for h in halves(x)], axis=2)
    drive_real = zoh_real[..., None] * input_real - zoh_imag[..., None] * input_imaginary
    drive_imag = zoh_real[..., None] * input_imaginary + zoh_imag[..., None] * input_real
    drive_real = drive_real.transpose(0, 2, 1)
    drive_imag = drive_imag.transpose(0, 2, 1)
    inv_real = inverse_real.transpose(1, 0, 2)
    inv_imag = inverse_imag.transpose(1, 0, 2)
    beside = lambda a, b: jnp.concatenate([a, b], axis=2)
    z1 = beside(inv_real, inv_real)
    z2 = beside(drive_real, drive_imag)
    z3 = beside(-inv_imag, inv_imag)
    z4 = beside(drive_imag, drive_real)
    dtab = jnp.concatenate([h for z in (z1, z2, z3, z4) for h in halves(z)], axis=1)
    last_real, last_imag = power_real[-1], power_imag[-1]
    all_real, all_imag = last_real, last_imag
    for _ in range(chunks - 1):
        all_real, all_imag = (
            all_real * last_real - all_imag * last_imag,
            all_real * last_imag + all_imag * last_real,
        )
    pair = lambda r, i: (jnp.concatenate([r, r], axis=1), jnp.concatenate([-i, i], axis=1))
    return gtab, dtab, pair(last_real, last_imag), pair(all_real, all_imag)


def recur(
    state_input, state_gate, decay_real, decay_frequency, log_step, input_real, input_imaginary,
    output_real, output_imaginary, skip_weight, decay_shift,
):
    tok_rows = state_input.shape[0]
    groups, states = decay_real.shape
    chunks = tok_rows // CHUNK
    span = CHUNK * GROUP_CH
    states2 = 2 * states
    gtab, dtab, (a16, b16), (a_all, b_all) = tables(
        decay_real, decay_frequency, log_step, input_real, input_imaginary, output_real,
        output_imaginary, chunks,
    )
    sums = jnp.dot(
        decay_shift.reshape(groups * chunks, CHUNK), jnp.asarray(shift_matrix(states2)),
        precision=lax.Precision.HIGHEST,
    )
    relative = sums[:, :span]
    head = jnp.exp(sums[:, span : span + states2])
    whole_log = sums[:, span + states2 :]
    whole = jnp.exp(whole_log)
    tail = jnp.exp(whole_log - sums[:, span : span + states2])
    weight_out = jnp.exp(relative)
    tile = jnp.zeros((8, LANES), F32).at[0, :groups].set(jnp.sum(decay_shift, axis=1))
    u = (
        state_input.reshape(chunks, CHUNK, groups, GROUP_CH)
        .transpose(2, 0, 1, 3)
        .reshape(groups * chunks, span)
    )
    uw = (u.astype(F32) * jnp.exp(-relative)).astype(BF16)
    spread = spread_matrix()
    rows = groups * chunks
    intra, g_out, pushed, message = pl.pallas_call(
        local_kernel,
        out_shape=(
            jax.ShapeDtypeStruct((rows, span), F32),
            jax.ShapeDtypeStruct((groups, states2, span), BF16),
            jax.ShapeDtypeStruct((rows, states2), F32),
            jax.ShapeDtypeStruct((groups + 8, LANES), F32),
        ),
        in_specs=[VMEM] * 10,
        out_specs=(VMEM,) * 4,
        compiler_params=params(),
        name="state_local",
    )(uw, gtab, dtab, jnp.asarray(spread, BF16), jnp.asarray(spread.T, BF16), a16, b16, tail, whole, tile)
    count = lax.axis_size("sp")
    carry = pl.pallas_call(
        carry_kernel,
        out_shape=jax.ShapeDtypeStruct((groups, states2), F32),
        in_specs=[VMEM] * 3,
        out_specs=VMEM,
        scratch_shapes=[
            pltpu.VMEM((count, groups + 8, LANES), F32),
            pltpu.SemaphoreType.DMA((count,)),
            pltpu.SemaphoreType.DMA((count,)),
        ],
        compiler_params=params(2),
        name="state_carry",
    )(message, a_all, b_all)
    recurrent = pl.pallas_call(
        finish_kernel,
        out_shape=jax.ShapeDtypeStruct((rows, span), F32),
        in_specs=[VMEM] * 9,
        out_specs=VMEM,
        scratch_shapes=[pltpu.VMEM((rows, states2), F32)],
        compiler_params=params(),
        name="state_finish",
    )(carry, pushed, intra, g_out, weight_out, a16, b16, head, whole)
    recurrent = (
        recurrent.reshape(groups, chunks, CHUNK, GROUP_CH)
        .transpose(1, 2, 0, 3)
        .reshape(tok_rows, groups * GROUP_CH)
    )
    recurrent = recurrent + skip_weight.reshape(1, -1) * state_input.astype(F32)
    return (jax.nn.sigmoid(state_gate.astype(F32)) * jax.nn.gelu(recurrent)).astype(BF16)


def attend(query_rows_all, key_value, sink_logit, head_gate):
    tok_rows = query_rows_all.shape[0]
    kv_width = key_value.shape[1] // 2
    kv_heads = kv_width // HEAD_DIM
    group_size = Q_HEADS // KV_HEADS
    blocks = tok_rows // WINDOW
    previous = shifted(key_value[tok_rows - WINDOW :], "sp", 1)
    joined = jnp.concatenate([previous, key_value], axis=0).reshape(
        blocks + 1, WINDOW, 2 * kv_width
    )
    banded = jnp.concatenate([joined[:-1], joined[1:]], axis=1)
    key_band = banded[..., :kv_width].reshape(blocks, 2 * WINDOW, kv_heads, HEAD_DIM)
    value_band = banded[..., kv_width:].reshape(blocks, 2 * WINDOW, kv_heads, HEAD_DIM)
    query_heads = query_rows_all.reshape(blocks, WINDOW, kv_heads, group_size, HEAD_DIM)
    scores = jnp.einsum(
        "nqkgd,nskd->nkgqs", query_heads, key_band, preferred_element_type=jnp.float32
    ) * HEAD_DIM ** (-0.5)
    query_index = jnp.arange(WINDOW, dtype=jnp.int32)[:, None]
    column = jnp.arange(2 * WINDOW, dtype=jnp.int32)[None, :]
    distance = WINDOW + query_index - column
    block_start = (
        lax.axis_index("sp") * tok_rows
        + jnp.arange(blocks, dtype=jnp.int32)[:, None, None] * WINDOW
    )
    allowed = (distance >= 0) & (distance < WINDOW) & (block_start - WINDOW + column >= 0)
    scores = jnp.where(allowed[:, None, None], scores, NEG_FILL)
    sink_col = sink_logit.reshape(kv_heads, group_size)[None, :, :, None, None]
    maxima = jnp.maximum(jnp.max(scores, axis=-1, keepdims=True), sink_col)
    exponent = jnp.exp(scores - maxima)
    totals = jnp.sum(exponent, axis=-1, keepdims=True) + jnp.exp(sink_col - maxima)
    weights = (exponent / totals).astype(jnp.bfloat16)
    attended = jnp.einsum(
        "nkgqs,nskd->nqkgd", weights, value_band, preferred_element_type=jnp.float32
    ).reshape(tok_rows, -1)
    return (jax.nn.sigmoid(head_gate.astype(jnp.float32)) * attended).astype(jnp.bfloat16)


def on_device(
    hidden,
    query_weight,
    key_weight,
    value_weight,
    head_gate_weight,
    state_in_weight,
    state_gate_weight,
    sink_logit,
    decay_real,
    decay_frequency,
    log_step,
    input_real,
    input_imaginary,
    output_real,
    output_imaginary,
    skip_weight,
    decay_shift,
    head_out_weight,
    state_out_weight,
):
    weight_list = (
        query_weight,
        key_weight,
        value_weight,
        head_gate_weight,
        state_in_weight,
        state_gate_weight,
    )
    portion = gather_hidden(hidden)
    sums = tuple(
        (jnp.dot(portion, weight, preferred_element_type=jnp.float32) for weight in weight_list)
    )
    query_rows_all, key_rows, value_rows, head_gate, state_input, state_gate = tuple(
        (running.astype(jnp.bfloat16) for running in sums)
    )
    key_value = jnp.concatenate([key_rows, value_rows], axis=1)
    head_mixed = attend(query_rows_all, key_value, sink_logit, head_gate)
    state_mixed = recur(
        state_input,
        state_gate,
        decay_real,
        decay_frequency,
        log_step,
        input_real,
        input_imaginary,
        output_real,
        output_imaginary,
        skip_weight,
        decay_shift,
    )
    return project_out(head_mixed, state_mixed, head_out_weight, state_out_weight)


def solution(mesh):
    in_specs = (
        P("sp", "tp"),
        P(None, "tp"),
        P(None, "tp"),
        P(None, "tp"),
        P(None, "tp"),
        P(None, "tp"),
        P(None, "tp"),
        P("tp"),
        P("tp", None),
        P("tp", None),
        P("tp"),
        P("tp", None, None),
        P("tp", None, None),
        P("tp", None, None),
        P("tp", None, None),
        P("tp", None),
        P("tp", "sp"),
        P("tp", None),
        P("tp", None),
    )
    out_specs = P("sp", "tp")
    return jax.shard_map(
        on_device, mesh=mesh, in_specs=in_specs, out_specs=out_specs, check_vma=False
    )
```

```python
import jax
import jax.numpy as jnp
import numpy as np
from jax import lax
from jax.experimental import pallas as pl
from jax.experimental.pallas import tpu as pltpu
from jax.sharding import PartitionSpec as P

HEAD_DIM = 64
Q_HEADS = 16
KV_HEADS = 8
GROUP_CH = 16
WINDOW = 128
CHUNK = 16
LANES = 128

NEG_FILL = -1e30
MESH = pl.DeviceIdType.MESH
VMEM = pl.BlockSpec(memory_space=pltpu.VMEM)
BF16 = jnp.bfloat16
F32 = jnp.float32


def params(collective_id=None):
    extra = {} if collective_id is None else {"collective_id": collective_id, "has_side_effects": True}
    return pltpu.CompilerParams(vmem_limit_bytes=60 * 1024 * 1024, **extra)


def hidden_kernel(own_ref, full_ref, send_sem, recv_sem):
    me = lax.axis_index("tp")
    other = 1 - me
    width = own_ref.shape[1]
    barrier = pltpu.get_barrier_semaphore()
    pl.semaphore_signal(barrier, inc=1, device_id={"tp": other}, device_id_type=MESH)
    pl.semaphore_wait(barrier, 1)
    mine = pl.ds(pl.multiple_of(me * width, LANES), width)
    copy = pltpu.make_async_remote_copy(
        src_ref=own_ref,
        dst_ref=full_ref.at[:, mine],
        send_sem=send_sem,
        recv_sem=recv_sem,
        device_id={"tp": other},
        device_id_type=MESH,
    )
    copy.start()
    full_ref[:, mine] = own_ref[...]
    copy.wait()


def gather_hidden(hidden):
    rows, width = hidden.shape
    return pl.pallas_call(
        hidden_kernel,
        out_shape=jax.ShapeDtypeStruct((rows, 2 * width), hidden.dtype),
        in_specs=[VMEM],
        out_specs=VMEM,
        scratch_shapes=[pltpu.SemaphoreType.DMA, pltpu.SemaphoreType.DMA],
        compiler_params=params(0),
        name="hidden_exchange",
    )(hidden)


def output_kernel(head_ref, state_ref, how_ref, sow_ref, out_ref, away, landed, send_sem, recv_sem):
    me = lax.axis_index("tp")
    other = 1 - me
    rows, width = out_ref.shape
    pieces = away.shape[0]
    step = width // pieces
    barrier = pltpu.get_barrier_semaphore()
    pl.semaphore_signal(barrier, inc=1, device_id={"tp": other}, device_id_type=MESH)
    pl.semaphore_wait(barrier, 1)

    def product(owner, piece):
        columns = pl.ds(pl.multiple_of(owner * width + piece * step, LANES), step)
        return jnp.dot(head_ref[...], how_ref[:, columns], preferred_element_type=F32) + jnp.dot(
            state_ref[...], sow_ref[:, columns], preferred_element_type=F32
        )

    copies = [
        pltpu.make_async_remote_copy(
            src_ref=away.at[piece],
            dst_ref=landed.at[piece],
            send_sem=send_sem.at[piece],
            recv_sem=recv_sem.at[piece],
            device_id={"tp": other},
            device_id_type=MESH,
        )
        for piece in range(pieces)
    ]
    for piece in range(pieces):
        away[piece] = product(other, piece).astype(away.dtype)
        if piece > 0:
            copies[piece - 1].start()
    own = [product(me, 0)]
    copies[pieces - 1].start()
    for piece in range(pieces):
        total = own[0] if piece == 0 else product(me, piece)
        copies[piece].wait()
        out_ref[:, pl.ds(piece * step, step)] = (total + landed[piece].astype(F32)).astype(out_ref.dtype)


def project_out(head_mixed, state_mixed, head_out_weight, state_out_weight):
    rows = head_mixed.shape[0]
    width = head_out_weight.shape[1] // 2
    pieces = 4
    return pl.pallas_call(
        output_kernel,
        out_shape=jax.ShapeDtypeStruct((rows, width), BF16),
        in_specs=[VMEM] * 4,
        out_specs=VMEM,
        scratch_shapes=[
            pltpu.VMEM((pieces, rows, width // pieces), F32),
            pltpu.VMEM((pieces, rows, width // pieces), F32),
            pltpu.SemaphoreType.DMA((pieces,)),
            pltpu.SemaphoreType.DMA((pieces,)),
        ],
        compiler_params=params(1),
        name="output_projection",
    )(head_mixed, state_mixed, head_out_weight, state_out_weight)


def turn(value, same, swapped):
    return value * same + pltpu.roll(value, value.shape[1] // 2, 1) * swapped


def regroup(parts):
    block = lax.broadcasted_iota(jnp.int32, parts[0].shape, 1) // GROUP_CH
    parts = list(parts)
    for distance in (4, 2, 1):
        low = (block & distance) == 0
        amount = distance * GROUP_CH
        for i in range(len(parts)):
            if i & distance:
                continue
            first, second = parts[i], parts[i + distance]
            parts[i] = jnp.where(low, first, pltpu.roll(second, amount, 1))
            parts[i + distance] = jnp.where(low, pltpu.roll(first, LANES - amount, 1), second)
    return parts


def split(value):
    high = value.astype(BF16)
    return [high, (value - high.astype(F32)).astype(BF16)]


def local_kernel(
    state_ref, win_ref, x1g_ref, x3g_ref, x1d_ref, x3d_ref, inr_ref, ini_ref, outr_ref, outi_ref,
    zr_ref, zi_ref, et_ref, a16_ref, b16_ref, tail_ref, whole_ref, tile_ref,
    intra_ref, g_ref, pushed_ref, msg_ref, wide, uw,
):
    groups = zr_ref.shape[0]
    chunks = win_ref.shape[0] // groups
    span = win_ref.shape[1]
    per_tile = LANES // GROUP_CH
    for tile in range(groups // per_tile):
        wide[tile] = state_ref[:, pl.ds(tile * LANES, LANES)].astype(F32)
        for half in range(span // LANES):
            parts = regroup([
                wide[tile, pl.ds(half * per_tile + k, chunks, stride=CHUNK), :] for k in range(per_tile)
            ])
            for k in range(per_tile):
                rows = pl.ds((tile * per_tile + k) * chunks, chunks)
                columns = pl.ds(half * LANES, LANES)
                uw[rows, columns] = (parts[k] * win_ref[rows, columns]).astype(BF16)
    row = lax.broadcasted_iota(jnp.int32, (span, span), 0) // GROUP_CH
    column = lax.broadcasted_iota(jnp.int32, (span, span), 1) // GROUP_CH
    causal = row <= column
    batch = 4
    beside = lambda a, b: jnp.concatenate([a, b], axis=1)

    def table_of(g):
        one_row = pl.ds(g, 1)
        drive_in = beside(inr_ref[g], ini_ref[g])
        x2d = zr_ref[one_row, :] * drive_in + zi_ref[one_row, :] * beside(ini_ref[g], inr_ref[g])
        x4d = pltpu.roll(x2d, LANES // 2, 1)
        x2g = beside(outr_ref[g], outr_ref[g])
        x4g = beside(outi_ref[g], outi_ref[g])
        stack = lambda xs: jnp.concatenate([h for x in xs for h in split(x)], axis=0)
        return beside(
            stack([x1g_ref[g], x2g, x3g_ref[g], x4g]), stack([x1d_ref[g], x2d, x3d_ref[g], x4d])
        )

    def one(step, carry):
        ids = [step * batch + k for k in range(batch)]
        tall = [jnp.dot(et_ref[...], table_of(g), preferred_element_type=F32) for g in ids]
        both = [
            (x[:span] * x[span : 2 * span] + x[2 * span : 3 * span] * x[3 * span :]).astype(BF16)
            for x in tall
        ]
        out_side = [x[:, :LANES] for x in both]
        in_side = [x[:, LANES:] for x in both]
        for g, value in zip(ids, out_side):
            g_ref[g] = value
        table = [
            jnp.where(
                causal,
                lax.dot_general(a, b, (((1,), (1,)), ((), ())), preferred_element_type=F32),
                0.0,
            ).astype(BF16)
            for a, b in zip(in_side, out_side)
        ]
        for g, t, d in zip(ids, table, in_side):
            rows = pl.ds(pl.multiple_of(g * chunks, chunks), chunks)
            u = uw[rows, :]
            intra_ref[rows, :] = jnp.dot(u, t, preferred_element_type=F32)
            pushed_ref[rows, :] = jnp.dot(u, d, preferred_element_type=F32)
        return carry

    lax.fori_loop(0, groups // batch, one, 0)
    same, swapped = a16_ref[...], b16_ref[...]
    state = jnp.zeros((groups, pushed_ref.shape[1]), F32)
    for c in range(chunks):
        rows = pl.ds(c, groups, stride=chunks)
        local = tail_ref[rows, :] * turn(pushed_ref[rows, :], same, swapped)
        pushed_ref[rows, :] = local
        state = whole_ref[rows, :] * turn(state, same, swapped) + local
    msg_ref[:groups, :] = state
    msg_ref[groups:, :] = tile_ref[...]


def attend_block(block, first_device, query_ref, gate_ref, sink_ref, keys, values, head_ref):
    rows = pl.ds(block * WINDOW, WINDOW)
    band = pl.ds(block * WINDOW, 2 * WINDOW)
    query_index = lax.broadcasted_iota(jnp.int32, (WINDOW, 2 * WINDOW), 0)
    column = lax.broadcasted_iota(jnp.int32, (WINDOW, 2 * WINDOW), 1)
    distance = WINDOW + query_index - column
    allowed = (distance >= 0) & (distance < WINDOW)
    if block == 0:
        allowed = allowed & (column >= jnp.where(first_device, WINDOW, 0))
    group_size = Q_HEADS // KV_HEADS
    heads = query_ref.shape[1] // HEAD_DIM
    query, key, value = query_ref[rows, :], keys[band, :], values[band, :]
    gate = gate_ref[rows, :].astype(F32)
    results = []
    for head in range(heads):
        kv = head // group_size
        q = query[:, head * HEAD_DIM : (head + 1) * HEAD_DIM]
        k = key[:, kv * HEAD_DIM : (kv + 1) * HEAD_DIM]
        v = value[:, kv * HEAD_DIM : (kv + 1) * HEAD_DIM]
        scores = lax.dot_general(q, k, (((1,), (1,)), ((), ())), preferred_element_type=F32)
        scores = jnp.where(allowed, scores * HEAD_DIM ** (-0.5), NEG_FILL)
        sink = sink_ref[head]
        maxima = jnp.maximum(jnp.max(scores, axis=-1, keepdims=True), sink)
        exponent = jnp.exp(scores - maxima)
        totals = jnp.sum(exponent, axis=-1, keepdims=True) + jnp.exp(sink - maxima)
        weights = (exponent * (1.0 / totals)).astype(BF16)
        results.append(jnp.dot(weights, v, preferred_element_type=F32))
    attended = jnp.concatenate(results, axis=1)
    head_ref[rows, :] = (jax.nn.sigmoid(gate) * attended).astype(head_ref.dtype)


def carry_kernel(
    msg_ref, same_ref, swapped_ref, query_ref, key_ref, value_ref, gate_ref, sink_ref,
    carry_ref, head_ref, landed, keys, values, send_sem, recv_sem, halo_send, halo_recv,
):
    me = lax.axis_index("sp")
    count = lax.axis_size("sp")
    groups = carry_ref.shape[0]
    tok_rows = key_ref.shape[0]
    barrier = pltpu.get_barrier_semaphore()

    def greet(hop, x):
        pl.semaphore_signal(
            barrier, inc=1, device_id={"sp": lax.rem(me + hop, count)}, device_id_type=MESH
        )
        return x

    lax.fori_loop(1, count, greet, 0)
    pl.semaphore_wait(barrier, count - 1)

    def outgoing(target):
        return pltpu.make_async_remote_copy(
            src_ref=msg_ref,
            dst_ref=landed.at[me],
            send_sem=send_sem.at[target],
            recv_sem=recv_sem.at[me],
            device_id={"sp": target},
            device_id_type=MESH,
        )

    def incoming(source):
        return pltpu.make_async_remote_copy(
            src_ref=msg_ref,
            dst_ref=landed.at[source],
            send_sem=send_sem.at[source],
            recv_sem=recv_sem.at[source],
            device_id={"sp": source},
            device_id_type=MESH,
        )

    def halos(target):
        return [
            pltpu.make_async_remote_copy(
                src_ref=own.at[pl.ds(tok_rows - WINDOW, WINDOW)],
                dst_ref=band.at[pl.ds(0, WINDOW)],
                send_sem=halo_send.at[k],
                recv_sem=halo_recv.at[k],
                device_id={"sp": target},
                device_id_type=MESH,
            )
            for k, (own, band) in enumerate(((key_ref, keys), (value_ref, values)))
        ]

    @pl.when(me < count - 1)
    def _():
        for copy in halos(me + 1):
            copy.start()

    def send(target, x):
        outgoing(target).start()
        return x

    lax.fori_loop(me + 1, count, send, 0)
    own_rows = pl.ds(WINDOW, tok_rows)
    keys[own_rows, :] = key_ref[...]
    values[own_rows, :] = value_ref[...]

    @pl.when(me == 0)
    def _():
        keys[:WINDOW, :] = jnp.zeros((WINDOW, keys.shape[1]), keys.dtype)
        values[:WINDOW, :] = jnp.zeros((WINDOW, values.shape[1]), values.dtype)

    blocks = tok_rows // WINDOW
    for block in range(1, blocks):
        attend_block(block, me == 0, query_ref, gate_ref, sink_ref, keys, values, head_ref)

    @pl.when(me > 0)
    def _():
        for copy in halos(me):
            copy.wait_recv()

    attend_block(0, me == 0, query_ref, gate_ref, sink_ref, keys, values, head_ref)

    same, swapped = same_ref[...], swapped_ref[...]
    pick = lax.broadcasted_iota(jnp.int32, (groups, LANES), 0) == lax.broadcasted_iota(
        jnp.int32, (groups, LANES), 1
    )

    def absorb(source, state):
        incoming(source).wait_recv()
        shift_row = landed[source, pl.ds(groups, 1), :]
        total = jnp.sum(jnp.where(pick, shift_row, 0.0), axis=1, keepdims=True)
        return jnp.exp(total) * turn(state, same, swapped) + landed[source, pl.ds(0, groups), :]

    carry_ref[...] = lax.fori_loop(0, me, absorb, jnp.zeros(carry_ref.shape, F32))

    def drain(target, x):
        outgoing(target).wait_send()
        return x

    lax.fori_loop(me + 1, count, drain, 0)

    @pl.when(me < count - 1)
    def _():
        for copy in halos(me + 1):
            copy.wait_send()


def finish_kernel(
    carry_ref, pushed_ref, intra_ref, g_ref, wout_ref, a16_ref, b16_ref, head_ref, whole_ref,
    state_ref, gate_ref, skip_ref, mixed_ref, entry, grouped, rows_out,
):
    groups = g_ref.shape[0]
    chunks = pushed_ref.shape[0] // groups
    span = intra_ref.shape[1]
    per_tile = LANES // GROUP_CH
    same, swapped = a16_ref[...], b16_ref[...]
    state = carry_ref[...]
    for c in range(chunks):
        rows = pl.ds(c, groups, stride=chunks)
        entry[rows, :] = head_ref[rows, :] * state
        state = whole_ref[rows, :] * turn(state, same, swapped) + pushed_ref[rows, :]
    batch = 8

    def one(step, x):
        for k in range(batch):
            g = step * batch + k
            rows = pl.ds(pl.multiple_of(g * chunks, chunks), chunks)
            far = lax.dot_general(
                entry[rows, :].astype(BF16), g_ref[g], (((1,), (1,)), ((), ())),
                preferred_element_type=F32,
            )
            grouped[rows, :] = wout_ref[rows, :] * (intra_ref[rows, :] + far)
        return x

    lax.fori_loop(0, groups // batch, one, 0)
    for tile in range(groups // per_tile):
        lanes = pl.ds(tile * LANES, LANES)
        for half in range(span // LANES):
            columns = pl.ds(half * LANES, LANES)
            parts = regroup([
                grouped[pl.ds((tile * per_tile + k) * chunks, chunks), columns]
                for k in range(per_tile)
            ])
            for k in range(per_tile):
                rows_out[tile, pl.ds(half * per_tile + k, chunks, stride=CHUNK), :] = parts[k]
        recurrent = rows_out[tile] + skip_ref[:, lanes] * state_ref[:, lanes].astype(F32)
        gate = jax.nn.sigmoid(gate_ref[:, lanes].astype(F32))
        mixed_ref[:, lanes] = (gate * jax.nn.gelu(recurrent)).astype(mixed_ref.dtype)


def spread_matrix():
    span = CHUNK * GROUP_CH
    column = np.arange(span)
    by_step = (np.arange(CHUNK)[:, None] == column[None] // GROUP_CH).astype(np.float32)
    by_channel = (np.arange(GROUP_CH)[:, None] == column[None] % GROUP_CH).astype(np.float32)
    out = np.zeros((8 * CHUNK, 4 * span), np.float32)
    for kind in range(4):
        block = by_channel if kind % 2 else by_step
        for half in range(2):
            first = (2 * kind + half) * CHUNK
            out[first : first + CHUNK, kind * span : (kind + 1) * span] = block
    return out


def shift_matrix(states2):
    span = CHUNK * GROUP_CH
    step = np.arange(CHUNK)
    upto = (step[:, None] <= (np.arange(span) // GROUP_CH)[None]).astype(np.float32)
    ref = (step < CHUNK // 2).astype(np.float32)[:, None]
    relative = upto - ref
    return np.concatenate(
        [relative, np.repeat(ref, states2, 1), np.ones((CHUNK, states2), np.float32)], axis=1
    )


def tables(decay_real, decay_frequency, log_step, chunks):
    decay_real = jnp.concatenate([decay_real, decay_real], axis=1)
    decay_frequency = jnp.concatenate([decay_frequency, decay_frequency], axis=1)
    width = decay_real.shape[1]
    low = jnp.arange(width) < width // 2
    stepsize = jnp.exp(log_step)[:, None]
    log_magnitude = decay_real * stepsize
    rotation = decay_frequency * stepsize
    magnitude = jnp.exp(log_magnitude)
    base_real = magnitude * jnp.cos(rotation)
    base_imag = magnitude * jnp.sin(rotation)
    denominator = decay_real * decay_real + decay_frequency * decay_frequency
    less_real = base_real - 1.0
    zoh_real = (less_real * decay_real + base_imag * decay_frequency) / denominator
    zoh_imag = (base_imag * decay_real - less_real * decay_frequency) / denominator
    counter = jnp.arange(1, CHUNK + 1, dtype=F32)[None, :, None]
    angle = counter * rotation[:, None, :]
    cosine, sine = jnp.cos(angle), jnp.sin(angle)
    grow = jnp.exp(counter * log_magnitude[:, None, :])
    shrink = jnp.exp(-counter * log_magnitude[:, None, :])
    power_real, power_imag = grow * cosine, grow * sine
    x1g = jnp.where(low, power_real, -power_imag)
    x3g = jnp.where(low, -power_imag, -power_real)
    x1d = shrink * cosine
    x3d = jnp.where(low, shrink * sine, -(shrink * sine))
    last_real, last_imag = power_real[:, -1], power_imag[:, -1]
    all_real, all_imag = last_real, last_imag
    for _ in range(chunks - 1):
        all_real, all_imag = (
            all_real * last_real - all_imag * last_imag,
            all_real * last_imag + all_imag * last_real,
        )
    sign = lambda value: jnp.where(low, -value, value)
    return (
        (x1g, x3g, x1d, x3d, zoh_real, sign(zoh_imag)),
        (last_real, sign(last_imag)),
        (all_real, sign(all_imag)),
    )


def on_device(
    hidden,
    query_weight,
    key_weight,
    value_weight,
    head_gate_weight,
    state_in_weight,
    state_gate_weight,
    sink_logit,
    decay_real,
    decay_frequency,
    log_step,
    input_real,
    input_imaginary,
    output_real,
    output_imaginary,
    skip_weight,
    decay_shift,
    head_out_weight,
    state_out_weight,
):
    portion = gather_hidden(hidden)
    state_input, query, key, value, head_gate, state_gate = (
        jnp.dot(portion, weight, preferred_element_type=F32).astype(BF16)
        for weight in (
            state_in_weight, query_weight, key_weight, value_weight, head_gate_weight,
            state_gate_weight,
        )
    )
    tok_rows = hidden.shape[0]
    groups, states = decay_real.shape
    chunks = tok_rows // CHUNK
    span = CHUNK * GROUP_CH
    states2 = 2 * states
    rows = groups * chunks
    prepared, (a16, b16), (a_all, b_all) = tables(decay_real, decay_frequency, log_step, chunks)
    x1g, x3g, x1d, x3d, zoh_real, zoh_imag = prepared
    sums = jnp.dot(
        decay_shift.reshape(rows, CHUNK), jnp.asarray(shift_matrix(states2)),
        precision=lax.Precision.HIGHEST,
    )
    relative = sums[:, :span]
    head = jnp.exp(sums[:, span : span + states2])
    whole_log = sums[:, span + states2 :]
    whole = jnp.exp(whole_log)
    tail = jnp.exp(whole_log - sums[:, span : span + states2])
    weight_out, weight_in = jnp.exp(relative), jnp.exp(-relative)
    tile = jnp.pad(jnp.sum(decay_shift, axis=1)[None], ((0, 7), (0, LANES - groups)))
    intra, g_out, pushed, message = pl.pallas_call(
        local_kernel,
        out_shape=(
            jax.ShapeDtypeStruct((rows, span), F32),
            jax.ShapeDtypeStruct((groups, span, states2), BF16),
            jax.ShapeDtypeStruct((rows, states2), F32),
            jax.ShapeDtypeStruct((groups + 8, LANES), F32),
        ),
        in_specs=[VMEM] * 18,
        out_specs=(VMEM,) * 4,
        scratch_shapes=[
            pltpu.VMEM((groups * GROUP_CH // LANES, tok_rows, LANES), F32),
            pltpu.VMEM((rows, span), BF16),
        ],
        compiler_params=params(),
        name="state_local",
    )(
        state_input, weight_in, x1g, x3g, x1d, x3d, input_real.transpose(0, 2, 1),
        input_imaginary.transpose(0, 2, 1), output_real, output_imaginary, zoh_real, zoh_imag,
        jnp.asarray(spread_matrix().T, BF16), a16, b16, tail, whole, tile,
    )
    count = lax.axis_size("sp")
    carry, head_mixed = pl.pallas_call(
        carry_kernel,
        out_shape=(
            jax.ShapeDtypeStruct((groups, states2), F32),
            jax.ShapeDtypeStruct(query.shape, BF16),
        ),
        in_specs=[VMEM] * 7 + [pl.BlockSpec(memory_space=pltpu.SMEM)],
        out_specs=(VMEM, VMEM),
        scratch_shapes=[
            pltpu.VMEM((count, groups + 8, LANES), F32),
            pltpu.VMEM((WINDOW + tok_rows, key.shape[1]), BF16),
            pltpu.VMEM((WINDOW + tok_rows, key.shape[1]), BF16),
            pltpu.SemaphoreType.DMA((count,)),
            pltpu.SemaphoreType.DMA((count,)),
            pltpu.SemaphoreType.DMA((2,)),
            pltpu.SemaphoreType.DMA((2,)),
        ],
        compiler_params=params(2),
        name="carry_and_attention",
    )(message, a_all, b_all, query, key, value, head_gate, sink_logit)
    state_mixed = pl.pallas_call(
        finish_kernel,
        out_shape=jax.ShapeDtypeStruct((tok_rows, groups * GROUP_CH), BF16),
        in_specs=[VMEM] * 12,
        out_specs=VMEM,
        scratch_shapes=[
            pltpu.VMEM((rows, states2), F32),
            pltpu.VMEM((rows, span), F32),
            pltpu.VMEM((groups * GROUP_CH // LANES, tok_rows, LANES), F32),
        ],
        compiler_params=params(),
        name="state_finish",
    )(
        carry, pushed, intra, g_out, weight_out, a16, b16, head, whole, state_input, state_gate,
        skip_weight.reshape(1, -1),
    )
    return project_out(head_mixed, state_mixed, head_out_weight, state_out_weight)


def solution(mesh):
    in_specs = (
        P("sp", "tp"),
        P(None, "tp"),
        P(None, "tp"),
        P(None, "tp"),
        P(None, "tp"),
        P(None, "tp"),
        P(None, "tp"),
        P("tp"),
        P("tp", None),
        P("tp", None),
        P("tp"),
        P("tp", None, None),
        P("tp", None, None),
        P("tp", None, None),
        P("tp", None, None),
        P("tp", None),
        P("tp", "sp"),
        P("tp", None),
        P("tp", None),
    )
    out_specs = P("sp", "tp")
    return jax.shard_map(
        on_device, mesh=mesh, in_specs=in_specs, out_specs=out_specs, check_vma=False
    )
```
